32 devices in a mesh: fs: 4 (over z), rep: 4 (over y, x), tp: 2 (over core).
Axes of the slice: x: 2, y: 2, z: 4, core: 2. Of those that a mesh axis runs over, the one named last changes fastest.
Arguments:
- mixer_input: bfloat16 [32768, 2048], P(('fs', 'rep')), may hold values from -6 to 6
- value_cot: bfloat16 [32768, 2048], P(('fs', 'rep'), 'tp'), may hold values from -0.22097087 to 0.22097087
- gate_cot: bfloat16 [32768, 2048], P(('fs', 'rep'), 'tp'), may hold values from -0.22097087 to 0.22097087
- value_weight: float32 [2048, 2048], P('fs', 'tp'), may hold values from -0.125 to 0.125
- gate_weight: float32 [2048, 2048], P('fs', 'tp'), may hold values from -0.125 to 0.125
- value_basis: bfloat16 [2048, 256], replicated, may hold values from -0.8838835 to 0.8838835
- gate_basis: bfloat16 [2048, 256], replicated, may hold values from -0.8838835 to 0.8838835
- value_first: float32 [256, 2048], P('fs', 'tp'), may hold values from -6 to 6
- gate_first: float32 [256, 2048], P('fs', 'tp'), may hold values from -6 to 6
- value_second: float32 [256, 2048], P('fs', 'tp'), may hold values from 0.01 to 1
- gate_second: float32 [256, 2048], P('fs', 'tp'), may hold values from 0.01 to 1
Outputs:
- value_new: float32 [2048, 2048], P('fs', 'tp')
- gate_new: float32 [2048, 2048], P('fs', 'tp')
- value_copy: bfloat16 [2048, 2048], P(None, 'tp')
- gate_copy: bfloat16 [2048, 2048], P(None, 'tp')
- value_step: float32 [2048, 2048], P('fs', 'tp')
- gate_step: float32 [2048, 2048], P('fs', 'tp')
- value_first_new: float32 [256, 2048], P('fs', 'tp')
- gate_first_new: float32 [256, 2048], P('fs', 'tp')
- value_second_new: float32 [256, 2048], P('fs', 'tp')
- gate_second_new: float32 [256, 2048], P('fs', 'tp')
The draws below stay inside these ranges and needn't reach their ends.
All inputs are finite; a program needn't handle non-finite values.
Results may differ from the reference program's by a relative error of at most 0.0044.
Values may be sent and summed in bfloat16 or wider, within the bound.
A program may use at most 128 MiB of HBM per device.

```python
import math
import jax
import jax.numpy as jnp
from jax import lax

D = 2048
R = 256
TOKENS = 32768


def cot_helper(key, salt):
    key = jax.random.fold_in(key, salt)
    first_key, second_key = jax.random.split(key, 2)
    base = jnp.clip(jax.random.normal(first_key, (TOKENS, D), jnp.float32), -6.0, 6.0)
    ramp = jnp.exp(jnp.log(3.0) * jnp.arange(D, dtype=jnp.float32) / (D - 1))
    jitter = jnp.exp(jax.random.uniform(second_key, (D,), jnp.float32) * jnp.log(2.0))
    limit = 40.0 * TOKENS ** (-0.5)
    values = base * (ramp * jitter)[None, :] * TOKENS ** (-0.5)
    return jnp.clip(values, -limit, limit)


def basis_helper(key, salt):
    key = jax.random.fold_in(key, salt)
    first_key, second_key = jax.random.split(key, 2)
    base = jnp.clip(jax.random.normal(first_key, (D, R), jnp.float32), -6.0, 6.0)
    top = 4.0
    ramp = jnp.exp(jnp.log(top) * jnp.arange(D, dtype=jnp.float32) / (D - 1))
    jitter = jnp.exp(jax.random.uniform(second_key, (D,), jnp.float32) * jnp.log(2.0))
    limit = 40.0 * D ** (-0.5)
    values = base * (ramp * jitter)[:, None] * D ** (-0.5)
    return jnp.clip(values, -limit, limit)


def draw_value_cot(key, part):
    return cot_helper(key, 11).astype(jnp.bfloat16)


def draw_gate_cot(key, part):
    return cot_helper(key, 23).astype(jnp.bfloat16)


def draw_value_basis(key, part):
    return basis_helper(key, 37).astype(jnp.bfloat16)


def draw_gate_basis(key, part):
    return basis_helper(key, 41).astype(jnp.bfloat16)


def block_scale(key, shape, shards, least, largest):
    def one(position, parts):
        steps = jax.random.uniform(jax.random.fold_in(jax.random.fold_in(key, 6), position), (parts,), jnp.float32, least / len(shards), largest / len(shards))
        return jnp.repeat(jnp.exp(steps), shape[position] // parts).reshape((-1,) + (1,) * (len(shape) - position - 1))

    level = one(*shards[0])
    for cut in shards[1:]:
        level = level * one(*cut)
    return level


def normal_values(key, extent, deviation, reach, cuts=(), kind=jnp.bfloat16):
    loudness = block_scale(key, extent, cuts, -0.22, 0.18) if cuts else 1.0
    array = jax.random.normal(key, extent, jnp.float32) * deviation * loudness
    return jnp.minimum(jnp.maximum(array, -reach), reach).astype(kind)


def setup_inputs(seed: int = 0) -> dict:
    streams_of = jax.random.split(jax.random.key(seed), 12)
    mixer_input = normal_values(streams_of[0], (TOKENS, D), 1.0, 6.0, ((0, 16),))
    value_cot = draw_value_cot(jax.random.fold_in(streams_of[11], 71), 0)
    gate_cot = draw_gate_cot(jax.random.fold_in(streams_of[11], 71), 0)
    value_weight = normal_values(streams_of[3], (D, D), D ** -0.5, 0.125, ((0, 4), (1, 2)), jnp.float32)
    gate_weight = normal_values(streams_of[4], (D, D), D ** -0.5, 0.125, ((0, 4), (1, 2)), jnp.float32)
    value_basis = draw_value_basis(jax.random.fold_in(streams_of[11], 71), 0)
    gate_basis = draw_gate_basis(jax.random.fold_in(streams_of[11], 71), 0)
    value_first = normal_values(streams_of[7], (R, D), 1.0, 6.0, ((0, 4), (1, 2)), jnp.float32)
    gate_first = normal_values(streams_of[8], (R, D), 1.0, 6.0, ((0, 4), (1, 2)), jnp.float32)
    value_second = jnp.clip(jnp.exp(math.log(1.0) - 4.6051702 * jax.random.uniform(streams_of[9], (R, D), jnp.float32) ** block_scale(streams_of[9], (R, D), ((0, 4), (1, 2)), -0.2, 0.2)), 0.01, 1.0)
    gate_second = jnp.clip(jnp.exp(math.log(1.0) - 4.6051702 * jax.random.uniform(streams_of[10], (R, D), jnp.float32) ** block_scale(streams_of[10], (R, D), ((0, 4), (1, 2)), -0.2, 0.2)), 0.01, 1.0)
    return {"mixer_input": mixer_input, "value_cot": value_cot, "gate_cot": gate_cot, "value_weight": value_weight, "gate_weight": gate_weight, "value_basis": value_basis, "gate_basis": gate_basis, "value_first": value_first, "gate_first": gate_first, "value_second": value_second, "gate_second": gate_second}


learn_rate = 0.02

def one_role(mixer_input, cotangent, weight, basis, first, second):
    gradient = jnp.dot(mixer_input.T, cotangent, preferred_element_type=jnp.float32)
    projected = jnp.dot(basis.astype(jnp.float32).T, gradient, precision=lax.Precision.HIGHEST)
    first_new = 0.9 * first + 0.1 * projected
    second_new = 0.95 * second + 0.05 * projected * projected
    scaled = (first_new * lax.rsqrt(second_new)).astype(jnp.bfloat16)
    expanded = jnp.dot(basis, scaled, preferred_element_type=jnp.float32)
    direction = expanded * lax.rsqrt(jnp.mean(expanded * expanded) + 1e-06)
    updated = weight - learn_rate * direction
    return (updated, updated.astype(jnp.bfloat16), direction, first_new, second_new)

def reference(mixer_input, value_cot, gate_cot, value_weight, gate_weight, value_basis, gate_basis, value_first, gate_first, value_second, gate_second):
    v_out = one_role(mixer_input, value_cot, value_weight, value_basis, value_first, value_second)
    g_out = one_role(mixer_input, gate_cot, gate_weight, gate_basis, gate_first, gate_second)
    return (v_out[0], g_out[0], v_out[1], g_out[1], v_out[2], g_out[2], v_out[3], g_out[3], v_out[4], g_out[4])
```

```python
import functools

import jax
import jax.numpy as jnp
from jax import lax
from jax.experimental import pallas as pl
from jax.experimental.pallas import tpu as pltpu
from jax.sharding import PartitionSpec as P

learn_rate = 0.02
CHUNKS = 4
F32 = jnp.float32
BF16 = jnp.bfloat16


def dot(a, b):
    return jnp.dot(a, b, preferred_element_type=F32)


def dot_first(a, b):
    return lax.dot_general(a, b, (((0,), (0,)), ((), ())), preferred_element_type=F32)


def split(a):
    upper = a.astype(BF16)
    return upper, (a - upper.astype(F32)).astype(BF16)


def exchange(
    n_fs, n_rep, n_tp,
    mixer, value_cot, gate_cot, value_weight, gate_weight, value_basis, gate_basis,
    value_first, gate_first, value_second, gate_second,
    value_rows, gate_rows, scaled_out, projected_out, squares_out,
    x_buf, cot_buf, w_buf, w_half, basis_buf, gram, acc, part_in,
    mid, mid_in, proj_all, scaled, sq_buf,
    x_sem, w_sem, b_sem, own_sem,
    w1_send, w1_recv, w2_send, w2_recv,
    s1_send, s1_recv, s2_send, s2_recv, p_send, p_recv, a_send, a_recv, g_send, g_recv, q_send, q_recv,
):
    f, r, t = lax.axis_index("fs"), lax.axis_index("rep"), lax.axis_index("tp")
    cots = (value_cot, gate_cot)
    weights = (value_weight, gate_weight)
    bases = (value_basis, gate_basis)
    gathered = (value_rows, gate_rows)
    tokens = mixer.shape[0]
    chunk = tokens // CHUNKS
    rows = value_weight.shape[0]
    share = rows // n_rep
    width = acc.shape[2]
    per_role = n_rep // 2
    low = mid.shape[1]

    def fs_at(d):
        return lax.rem(f + d, n_fs)

    def rep_at(d):
        return lax.rem(r + d, n_rep)

    def send(src, dst, s, v, **where):
        return pltpu.make_async_remote_copy(
            src_ref=src, dst_ref=dst, send_sem=s, recv_sem=v,
            device_id=where, device_id_type=pl.DeviceIdType.MESH,
        )

    w_loads = [pltpu.make_async_copy(weights[k], w_buf.at[k], w_sem.at[k]) for k in range(2)]
    b_loads = [pltpu.make_async_copy(bases[k], basis_buf.at[k], b_sem.at[k]) for k in range(2)]

    def x_loads(c):
        span = pl.ds(pl.multiple_of(c * chunk, chunk), chunk)
        return [pltpu.make_async_copy(mixer.at[span], x_buf.at[c], x_sem.at[c, 0])] + [
            pltpu.make_async_copy(cots[k].at[span], cot_buf.at[k, c], x_sem.at[c, 1 + k]) for k in range(2)
        ]

    for copy in w_loads + b_loads:
        copy.start()
    for c in range(CHUNKS):
        for copy in x_loads(c):
            copy.start()

    barrier = pltpu.get_barrier_semaphore()
    for d in range(1, n_fs):
        pl.semaphore_signal(barrier, inc=1, device_id={"fs": fs_at(d)}, device_id_type=pl.DeviceIdType.MESH)
    for d in range(1, n_rep):
        pl.semaphore_signal(barrier, inc=1, device_id={"rep": rep_at(d)}, device_id_type=pl.DeviceIdType.MESH)
    for d in range(1, n_tp):
        pl.semaphore_signal(
            barrier, inc=1, device_id={"tp": lax.rem(t + d, n_tp)}, device_id_type=pl.DeviceIdType.MESH
        )
    for k in range(2):
        w_loads[k].wait()
        w_half[k] = w_buf[k].astype(BF16)
    pl.semaphore_wait(barrier, n_fs + n_rep + n_tp - 3)

    def share_of(block, part_index):
        return pl.ds(pl.multiple_of(block * rows + part_index * share, share), share)

    w1 = {}
    for d in range(1, n_fs):
        for k in range(2):
            w1[d, k] = send(
                w_half.at[k, pl.ds(pl.multiple_of(r * share, share), share)],
                gathered[k].at[share_of(f, r)],
                w1_send.at[d - 1, k], w1_recv.at[d - 1, k], fs=fs_at(d),
            )
            w1[d, k].start()
    own = []
    for k in range(2):
        copy = pltpu.make_async_copy(
            w_half.at[k], gathered[k].at[pl.ds(pl.multiple_of(f * rows, rows), rows)], own_sem.at[k]
        )
        copy.start()
        own.append(copy)

    for copy in b_loads:
        copy.wait()
    acc[...] = jnp.zeros_like(acc)

    def one_chunk(c, carry):
        for copy in x_loads(c):
            copy.wait()
        x = x_buf[c]
        for k in range(2):
            upper, lower = split(dot(x, basis_buf[k]))
            for q in range(per_role):
                cols = slice(q * width, (q + 1) * width)
                cot = cot_buf[k, c, :, cols]
                acc[k * per_role + q] += dot_first(upper, cot) + dot_first(lower, cot)
        return carry

    lax.fori_loop(0, CHUNKS, one_chunk, 0)
    s1 = {}
    for d in range(1, n_rep):
        s1[d] = send(
            acc.at[rep_at(d)], part_in.at[d - 1], s1_send.at[d - 1], s1_recv.at[d - 1], rep=rep_at(d)
        )
        s1[d].start()

    w2 = {}

    def forward(d):
        source = lax.rem(f - d + n_fs, n_fs)
        for k in range(2):
            w1[d, k].wait_recv()
            for e in range(1, n_rep):
                rows_ref = gathered[k].at[share_of(source, r)]
                w2[d, e, k] = send(
                    rows_ref, rows_ref, w2_send.at[d - 1, e - 1, k], w2_recv.at[d - 1, e - 1, k], rep=rep_at(e)
                )
                w2[d, e, k].start()

    forward(1)
    for k in range(2):
        upper, lower = split(dot_first(basis_buf[k], basis_buf[k]))
        gram[k, 0] = upper
        gram[k, 1] = lower

    for d in range(1, n_rep):
        s1[d].wait_recv()
    total = acc[r]
    for d in range(1, n_rep):
        total += part_in[d - 1]
    mid[...] = total.reshape(mid.shape)
    s2 = {}
    for d in range(1, n_fs):
        s2[d] = send(
            mid.at[fs_at(d)], mid_in.at[d - 1], s2_send.at[d - 1], s2_recv.at[d - 1], fs=fs_at(d)
        )
        s2[d].start()
    for d in range(2, n_fs - 1):
        forward(d)
    for d in range(1, n_fs):
        s2[d].wait_recv()
    small = mid[f]
    for d in range(1, n_fs):
        small += mid_in[d - 1]
    proj_all[r] = small

    cols = pl.ds(pl.multiple_of(lax.rem(r, per_role) * width, width), width)
    is_value = r < per_role
    first = jnp.where(is_value, value_first[:, cols], gate_first[:, cols])
    second = jnp.where(is_value, value_second[:, cols], gate_second[:, cols])
    first_new = 0.9 * first + 0.1 * small
    second_new = 0.95 * second + 0.05 * small * small
    scaled[r, f] = (first_new * lax.rsqrt(second_new)).astype(BF16)
    a4, p4, g4 = {}, {}, {}
    for d in range(1, n_fs):
        a4[d] = send(
            scaled.at[r, f], scaled.at[r, f], a_send.at[d - 1], a_recv.at[d - 1], fs=fs_at(d)
        )
        a4[d].start()
    for d in range(1, n_rep):
        p4[d] = send(proj_all.at[r], proj_all.at[r], p_send.at[d - 1], p_recv.at[d - 1], rep=rep_at(d))
        p4[d].start()
    if n_fs > 2:
        forward(n_fs - 1)
    for d in range(1, n_fs):
        a4[d].wait_recv()
    for d in range(1, n_rep):
        g4[d] = send(scaled.at[r], scaled.at[r], g_send.at[d - 1], g_recv.at[d - 1], rep=rep_at(d))
        g4[d].start()
    for d in range(1, n_rep):
        g4[d].wait_recv()

    for k in range(2):
        squares = 0.0
        for q in range(per_role):
            s = scaled[k * per_role + q].reshape(n_fs * low, width)
            squares += jnp.sum((dot(gram[k, 0], s) + dot(gram[k, 1], s)) * s.astype(F32))
        sq_buf[0, k] = jnp.full(sq_buf.shape[2:], squares, F32)
    q4 = []
    for d in range(1, n_tp):
        copy = send(
            sq_buf.at[0], sq_buf.at[d], q_send.at[d - 1], q_recv.at[d - 1], tp=lax.rem(t + d, n_tp)
        )
        copy.start()
        q4.append(copy)
    for d in range(1, n_rep):
        p4[d].wait_recv()
    scaled_out[...] = scaled[...].reshape(scaled_out.shape)
    projected_out[...] = proj_all[...]
    for copy in q4:
        copy.wait_recv()
    sums = sq_buf[0]
    for d in range(1, n_tp):
        sums += sq_buf[d]
    squares_out[...] = sums

    for copy in list(w1.values()) + list(s1.values()) + list(s2.values()) + list(a4.values()):
        copy.wait_send()
    for copy in list(p4.values()) + list(g4.values()) + q4:
        copy.wait_send()
    for copy in own:
        copy.wait()
    for copy in w2.values():
        copy.wait()


def finish(
    own_blocks, entries,
    where, value_rows, gate_rows, value_basis, gate_basis, value_weight, gate_weight,
    scaled, projected, squares, value_first, gate_first, value_second, gate_second,
    value_new, gate_new, value_copy, gate_copy, value_step, gate_step,
    value_first_new, gate_first_new, value_second_new, gate_second_new,
):
    step = pl.program_id(0)
    width = scaled.shape[2]
    per_role = scaled.shape[0] // 2
    roles = (
        (value_rows, value_basis, value_weight, value_new, value_copy, value_step),
        (gate_rows, gate_basis, gate_weight, gate_new, gate_copy, gate_step),
    )
    for k, (rows, basis, weight, new, copy, step_out) in enumerate(roles):
        factor = lax.rsqrt(squares[k, :1, :1] / entries + 1e-06)
        for q in range(per_role):
            cols = slice(q * width, (q + 1) * width)
            direction = dot(basis[...], scaled[k * per_role + q]) * factor
            copy[:, cols] = (rows[:, cols].astype(F32) - learn_rate * direction).astype(BF16)

            @pl.when(step < own_blocks)
            def _():
                step_out[:, cols] = direction
                new[:, cols] = weight[:, cols] - learn_rate * direction

    @pl.when(step == 0)
    def _():
        moments = (
            (value_first, value_second, value_first_new, value_second_new),
            (gate_first, gate_second, gate_first_new, gate_second_new),
        )
        for k, (first, second, first_new, second_new) in enumerate(moments):
            for q in range(per_role):
                cols = slice(q * width, (q + 1) * width)
                small = projected[k * per_role + q]
                first_new[:, cols] = 0.9 * first[:, cols] + 0.1 * small
                second_new[:, cols] = 0.95 * second[:, cols] + 0.05 * small * small


def local(sizes, *args):
    n_fs, n_rep, n_tp = sizes
    (mixer, value_cot, gate_cot, value_weight, gate_weight, value_basis, gate_basis,
     value_first, gate_first, value_second, gate_second) = args
    tokens, model = mixer.shape
    half = value_cot.shape[1]
    rows = value_weight.shape[0]
    rank = value_basis.shape[1]
    low = value_first.shape[0]
    width = 2 * half // n_rep
    chunk = tokens // CHUNKS
    any_spec = pl.BlockSpec(memory_space=pl.ANY)
    vmem = pl.BlockSpec(memory_space=pltpu.VMEM)
    dma = pltpu.SemaphoreType.DMA
    scratch = [
        pltpu.VMEM((CHUNKS, chunk, model), BF16),
        pltpu.VMEM((2, CHUNKS, chunk, half), BF16),
        pltpu.VMEM((2, rows, half), F32),
        pltpu.VMEM((2, rows, half), BF16),
        pltpu.VMEM((2, model, rank), BF16),
        pltpu.VMEM((2, 2, rank, rank), BF16),
        pltpu.VMEM((n_rep, rank, width), F32),
        pltpu.VMEM((n_rep - 1, rank, width), F32),
        pltpu.VMEM((n_fs, low, width), F32),
        pltpu.VMEM((n_fs - 1, low, width), F32),
        pltpu.VMEM((n_rep, low, width), F32),
        pltpu.VMEM((n_rep, n_fs, low, width), BF16),
        pltpu.VMEM((n_tp, 2, 8, 128), F32),
        dma((CHUNKS, 3)), dma((2,)), dma((2,)), dma((2,)),
        dma((n_fs - 1, 2)), dma((n_fs - 1, 2)),
        dma((n_fs - 1, n_rep - 1, 2)), dma((n_fs - 1, n_rep - 1, 2)),
    ]
    for count in (n_rep, n_fs, n_rep, n_fs, n_rep, n_tp):
        scratch += [dma((count - 1,)), dma((count - 1,))]
    value_rows, gate_rows, scaled, projected, squares = pl.pallas_call(
        functools.partial(exchange, n_fs, n_rep, n_tp),
        out_shape=(
            jax.ShapeDtypeStruct((rows * n_fs, half), BF16),
            jax.ShapeDtypeStruct((rows * n_fs, half), BF16),
            jax.ShapeDtypeStruct((n_rep, rank, width), BF16),
            jax.ShapeDtypeStruct((n_rep, low, width), F32),
            jax.ShapeDtypeStruct((2, 8, 128), F32),
        ),
        in_specs=[any_spec] * 7 + [vmem] * 4,
        out_specs=(any_spec, any_spec, vmem, vmem, vmem),
        scratch_shapes=scratch,
        compiler_params=pltpu.CompilerParams(
            collective_id=0, has_side_effects=True, vmem_limit_bytes=52 * 1024 * 1024
        ),
        name="exchange",
    )(*args)

    block = min(rows, 256)
    own_blocks = rows // block
    blocks = model // block
    where = (lax.axis_index("fs") * own_blocks).astype(jnp.int32).reshape(1)

    def turned(i, w):
        return (lax.rem(w[0] + i, blocks), 0)

    def own(i, w):
        return (jnp.minimum(i, own_blocks - 1), 0)

    def whole(shape):
        return pl.BlockSpec(shape, lambda i, w: (0,) * len(shape))

    row_spec = pl.BlockSpec((block, half), turned)
    basis_spec = pl.BlockSpec((block, rank), turned)
    own_spec = pl.BlockSpec((block, half), own)
    moment = whole((low, half))
    return pl.pallas_call(
        functools.partial(finish, own_blocks, float(model) * half * n_tp),
        grid_spec=pltpu.PrefetchScalarGridSpec(
            num_scalar_prefetch=1,
            grid=(blocks,),
            in_specs=[row_spec, row_spec, basis_spec, basis_spec, own_spec, own_spec,
                      whole(scaled.shape), whole(projected.shape), whole(squares.shape)] + [moment] * 4,
            out_specs=[own_spec, own_spec, row_spec, row_spec, own_spec, own_spec] + [moment] * 4,
        ),
        out_shape=[
            jax.ShapeDtypeStruct((rows, half), F32),
            jax.ShapeDtypeStruct((rows, half), F32),
            jax.ShapeDtypeStruct((model, half), BF16),
            jax.ShapeDtypeStruct((model, half), BF16),
            jax.ShapeDtypeStruct((rows, half), F32),
            jax.ShapeDtypeStruct((rows, half), F32),
        ] + [jax.ShapeDtypeStruct((low, half), F32)] * 4,
        compiler_params=pltpu.CompilerParams(vmem_limit_bytes=40 * 1024 * 1024),
        name="finish",
    )(where, value_rows, gate_rows, value_basis, gate_basis, value_weight, gate_weight,
      scaled, projected, squares, value_first, gate_first, value_second, gate_second)


def solution(mesh):
    sizes = tuple(mesh.shape[name] for name in ("fs", "rep", "tp"))
    return jax.shard_map(
        lambda *args: tuple(local(sizes, *args)),
        mesh=mesh,
        in_specs=(
            P(("fs", "rep"), None),
            P(("fs", "rep"), "tp"),
            P(("fs", "rep"), "tp"),
            P("fs", "tp"),
            P("fs", "tp"),
            P(),
            P(),
            P("fs", "tp"),
            P("fs", "tp"),
            P("fs", "tp"),
            P("fs", "tp"),
        ),
        out_specs=(
            P("fs", "tp"),
            P("fs", "tp"),
            P(None, "tp"),
            P(None, "tp"),
            P("fs", "tp"),
            P("fs", "tp"),
            P("fs", "tp"),
            P("fs", "tp"),
            P("fs", "tp"),
            P("fs", "tp"),
        ),
        check_vma=False,
    )
```

```python
import functools

import jax
import jax.numpy as jnp
from jax import lax
from jax.experimental import pallas as pl
from jax.experimental.pallas import tpu as pltpu
from jax.sharding import PartitionSpec as P

learn_rate = 0.02
CHUNKS = 4
F32 = jnp.float32
BF16 = jnp.bfloat16


def dot(a, b):
    return jnp.dot(a, b, preferred_element_type=F32)


def dot_first(a, b):
    return lax.dot_general(a, b, (((0,), (0,)), ((), ())), preferred_element_type=F32)


def split(a):
    upper = a.astype(BF16)
    return upper, (a - upper.astype(F32)).astype(BF16)


def exchange(
    n_fs, n_rep, n_tp,
    mixer, value_cot, gate_cot, value_weight, gate_weight, value_basis, gate_basis,
    value_first_hbm, gate_first_hbm, value_second_hbm, gate_second_hbm,
    value_rows, gate_rows, scaled_out, projected_out, squares_out,
    x_buf, cot_buf, w_buf, w_half, basis_buf, gram, acc, part_in,
    mid, mid_in, proj_all, scaled, sq_buf, moments,
    x_sem, w_sem, b_sem, own_sem, m_sem,
    w1_send, w1_recv, w2_send, w2_recv,
    s1_send, s1_recv, s2_send, s2_recv, p_send, p_recv, a_send, a_recv, g_send, g_recv, q_send, q_recv,
):
    f, r, t = lax.axis_index("fs"), lax.axis_index("rep"), lax.axis_index("tp")
    cots = (value_cot, gate_cot)
    weights = (value_weight, gate_weight)
    bases = (value_basis, gate_basis)
    gathered = (value_rows, gate_rows)
    tokens = mixer.shape[0]
    chunk = tokens // CHUNKS
    rows = value_weight.shape[0]
    share = rows // n_rep
    width = acc.shape[2]
    per_role = n_rep // 2
    low = mid.shape[1]

    def fs_at(d):
        return lax.rem(f + d, n_fs)

    def rep_at(d):
        return lax.rem(r + d, n_rep)

    def send(src, dst, s, v, **where):
        return pltpu.make_async_remote_copy(
            src_ref=src, dst_ref=dst, send_sem=s, recv_sem=v,
            device_id=where, device_id_type=pl.DeviceIdType.MESH,
        )

    w_loads = [pltpu.make_async_copy(weights[k], w_buf.at[k], w_sem.at[k]) for k in range(2)]
    b_loads = [pltpu.make_async_copy(bases[k], basis_buf.at[k], b_sem.at[k]) for k in range(2)]

    def x_loads(c):
        span = pl.ds(pl.multiple_of(c * chunk, chunk), chunk)
        return [pltpu.make_async_copy(mixer.at[span], x_buf.at[c], x_sem.at[c, 0])] + [
            pltpu.make_async_copy(cots[k].at[span], cot_buf.at[k, c], x_sem.at[c, 1 + k]) for k in range(2)
        ]

    m_loads = [
        pltpu.make_async_copy(ref, moments.at[i], m_sem.at[i])
        for i, ref in enumerate((value_first_hbm, gate_first_hbm, value_second_hbm, gate_second_hbm))
    ]
    for copy in w_loads + b_loads:
        copy.start()
    for c in range(CHUNKS):
        for copy in x_loads(c):
            copy.start()

    for copy in m_loads:
        copy.start()

    barrier = pltpu.get_barrier_semaphore()
    for d in range(1, n_fs):
        pl.semaphore_signal(barrier, inc=1, device_id={"fs": fs_at(d)}, device_id_type=pl.DeviceIdType.MESH)
    for d in range(1, n_rep):
        pl.semaphore_signal(barrier, inc=1, device_id={"rep": rep_at(d)}, device_id_type=pl.DeviceIdType.MESH)
    for d in range(1, n_tp):
        pl.semaphore_signal(
            barrier, inc=1, device_id={"tp": lax.rem(t + d, n_tp)}, device_id_type=pl.DeviceIdType.MESH
        )
    for k in range(2):
        w_loads[k].wait()
        w_half[k] = w_buf[k].astype(BF16)
    pl.semaphore_wait(barrier, n_fs + n_rep + n_tp - 3)

    def share_of(block, part_index):
        return pl.ds(pl.multiple_of(block * rows + part_index * share, share), share)

    w1 = {}
    for d in range(1, n_fs):
        for k in range(2):
            w1[d, k] = send(
                w_half.at[k, pl.ds(pl.multiple_of(r * share, share), share)],
                gathered[k].at[share_of(f, r)],
                w1_send.at[d - 1, k], w1_recv.at[d - 1, k], fs=fs_at(d),
            )
            w1[d, k].start()
    own = []
    for k in range(2):
        copy = pltpu.make_async_copy(
            w_half.at[k], gathered[k].at[pl.ds(pl.multiple_of(f * rows, rows), rows)], own_sem.at[k]
        )
        copy.start()
        own.append(copy)

    for copy in b_loads:
        copy.wait()
    acc[...] = jnp.zeros_like(acc)

    def one_chunk(c, carry):
        for copy in x_loads(c):
            copy.wait()
        x = x_buf[c]
        for k in range(2):
            upper, lower = split(dot(x, basis_buf[k]))
            for q in range(per_role):
                cols = slice(q * width, (q + 1) * width)
                cot = cot_buf[k, c, :, cols]
                acc[k * per_role + q] += dot_first(upper, cot) + dot_first(lower, cot)
        return carry

    lax.fori_loop(0, CHUNKS, one_chunk, 0)
    s1 = {}
    for d in range(1, n_rep):
        s1[d] = send(
            acc.at[rep_at(d)], part_in.at[d - 1], s1_send.at[d - 1], s1_recv.at[d - 1], rep=rep_at(d)
        )
        s1[d].start()

    w2, heard = {}, set()
    near, far = (r + 1 - 2 * lax.rem(r, 2), lax.rem(r + 2, n_rep)) if n_rep == 4 else (None, None)

    def pass_on(d, e, k, owner, peer):
        source = lax.rem(f - d + n_fs, n_fs)
        rows_ref = gathered[k].at[share_of(source, owner)]
        w2[d, e, k] = send(
            rows_ref, rows_ref, w2_send.at[d - 1, e, k], w2_recv.at[d - 1, e, k], rep=peer
        )
        w2[d, e, k].start()

    def forward(d):
        for k in range(2):
            w1[d, k].wait_recv()
            peers = (near, far) if n_rep == 4 else [rep_at(e) for e in range(1, n_rep)]
            for e, peer in enumerate(peers):
                pass_on(d, e, k, r, peer)

    def relay(d):
        if n_rep == 4:
            for e, k, owner, peer in ((0, 0, near, far), (1, 1, far, near)):
                w2[d, e, k].wait_recv()
                heard.add((d, e, k))
                pass_on(d, 2, k, owner, peer)

    forward(1)
    for k in range(2):
        upper, lower = split(dot_first(basis_buf[k], basis_buf[k]))
        gram[k, 0] = upper
        gram[k, 1] = lower

    for d in range(1, n_rep):
        s1[d].wait_recv()
    total = acc[r]
    for d in range(1, n_rep):
        total += part_in[d - 1]
    mid[...] = total.reshape(mid.shape)
    s2 = {}
    for d in range(1, n_fs):
        s2[d] = send(
            mid.at[fs_at(d)], mid_in.at[d - 1], s2_send.at[d - 1], s2_recv.at[d - 1], fs=fs_at(d)
        )
        s2[d].start()
    for d in range(2, n_fs - 1):
        forward(d)
        relay(d - 1)
    for d in range(1, n_fs):
        s2[d].wait_recv()
    small = mid[f]
    for d in range(1, n_fs):
        small += mid_in[d - 1]
    proj_all[r] = small.astype(BF16)

    cols = pl.ds(pl.multiple_of(lax.rem(r, per_role) * width, width), width)
    is_value = r < per_role
    for copy in m_loads:
        copy.wait()
    first = jnp.where(is_value, moments[0, :, cols], moments[1, :, cols])
    second = jnp.where(is_value, moments[2, :, cols], moments[3, :, cols])
    first_new = 0.9 * first + 0.1 * small
    second_new = 0.95 * second + 0.05 * small * small
    scaled[r, f] = (first_new * lax.rsqrt(second_new)).astype(BF16)
    a4, p4, g4 = {}, {}, {}
    for d in range(1, n_fs):
        a4[d] = send(
            scaled.at[r, f], scaled.at[r, f], a_send.at[d - 1], a_recv.at[d - 1], fs=fs_at(d)
        )
        a4[d].start()
    for d in range(1, n_rep):
        p4[d] = send(proj_all.at[r], proj_all.at[r], p_send.at[d - 1], p_recv.at[d - 1], rep=rep_at(d))
        p4[d].start()
    if n_fs > 2:
        forward(n_fs - 1)
        relay(n_fs - 2)
    for d in range(1, n_fs):
        a4[d].wait_recv()
    for d in range(1, n_rep):
        g4[d] = send(scaled.at[r], scaled.at[r], g_send.at[d - 1], g_recv.at[d - 1], rep=rep_at(d))
        g4[d].start()
    relay(n_fs - 1)
    for d in range(1, n_rep):
        g4[d].wait_recv()

    for k in range(2):
        squares = 0.0
        for q in range(per_role):
            s = scaled[k * per_role + q].reshape(n_fs * low, width)
            squares += jnp.sum((dot(gram[k, 0], s) + dot(gram[k, 1], s)) * s.astype(F32))
        sq_buf[0, k] = jnp.full(sq_buf.shape[2:], squares, F32)
    q4 = []
    for d in range(1, n_tp):
        copy = send(
            sq_buf.at[0], sq_buf.at[d], q_send.at[d - 1], q_recv.at[d - 1], tp=lax.rem(t + d, n_tp)
        )
        copy.start()
        q4.append(copy)
    for d in range(1, n_rep):
        p4[d].wait_recv()
    scaled_out[...] = scaled[...].reshape(scaled_out.shape)
    projected_out[...] = proj_all[...]
    for copy in q4:
        copy.wait_recv()
    sums = sq_buf[0]
    for d in range(1, n_tp):
        sums += sq_buf[d]
    squares_out[...] = sums

    for copy in list(w1.values()) + list(s1.values()) + list(s2.values()) + list(a4.values()):
        copy.wait_send()
    for copy in list(p4.values()) + list(g4.values()) + q4:
        copy.wait_send()
    for copy in own:
        copy.wait()
    for key, copy in w2.items():
        copy.wait_send()
        if key not in heard:
            copy.wait_recv()


def finish(
    own_blocks, entries,
    where, value_rows, gate_rows, value_basis, gate_basis, value_weight, gate_weight,
    scaled, projected, squares, value_first, gate_first, value_second, gate_second,
    value_new, gate_new, value_copy, gate_copy, value_step, gate_step,
    value_first_new, gate_first_new, value_second_new, gate_second_new,
):
    step = pl.program_id(0)
    width = scaled.shape[2]
    per_role = scaled.shape[0] // 2
    roles = (
        (value_rows, value_basis, value_weight, value_new, value_copy, value_step),
        (gate_rows, gate_basis, gate_weight, gate_new, gate_copy, gate_step),
    )
    for k, (rows, basis, weight, new, copy, step_out) in enumerate(roles):
        factor = lax.rsqrt(squares[k, :1, :1] / entries + 1e-06)
        for q in range(per_role):
            cols = slice(q * width, (q + 1) * width)
            direction = dot(basis[...], scaled[k * per_role + q]) * factor
            copy[:, cols] = (rows[:, cols].astype(F32) - learn_rate * direction).astype(BF16)

            @pl.when(step < own_blocks)
            def _():
                step_out[:, cols] = direction
                new[:, cols] = weight[:, cols] - learn_rate * direction

    @pl.when(step == 0)
    def _():
        moments = (
            (value_first, value_second, value_first_new, value_second_new),
            (gate_first, gate_second, gate_first_new, gate_second_new),
        )
        for k, (first, second, first_new, second_new) in enumerate(moments):
            for q in range(per_role):
                cols = slice(q * width, (q + 1) * width)
                small = projected[k * per_role + q].astype(F32)
                first_new[:, cols] = 0.9 * first[:, cols] + 0.1 * small
                second_new[:, cols] = 0.95 * second[:, cols] + 0.05 * small * small


def local(sizes, *args):
    n_fs, n_rep, n_tp = sizes
    (mixer, value_cot, gate_cot, value_weight, gate_weight, value_basis, gate_basis,
     value_first, gate_first, value_second, gate_second) = args
    tokens, model = mixer.shape
    half = value_cot.shape[1]
    rows = value_weight.shape[0]
    rank = value_basis.shape[1]
    low = value_first.shape[0]
    width = 2 * half // n_rep
    chunk = tokens // CHUNKS
    any_spec = pl.BlockSpec(memory_space=pl.ANY)
    vmem = pl.BlockSpec(memory_space=pltpu.VMEM)
    dma = pltpu.SemaphoreType.DMA
    scratch = [
        pltpu.VMEM((CHUNKS, chunk, model), BF16),
        pltpu.VMEM((2, CHUNKS, chunk, half), BF16),
        pltpu.VMEM((2, rows, half), F32),
        pltpu.VMEM((2, rows, half), BF16),
        pltpu.VMEM((2, model, rank), BF16),
        pltpu.VMEM((2, 2, rank, rank), BF16),
        pltpu.VMEM((n_rep, rank, width), F32),
        pltpu.VMEM((n_rep - 1, rank, width), F32),
        pltpu.VMEM((n_fs, low, width), F32),
        pltpu.VMEM((n_fs - 1, low, width), F32),
        pltpu.VMEM((n_rep, low, width), BF16),
        pltpu.VMEM((n_rep, n_fs, low, width), BF16),
        pltpu.VMEM((n_tp, 2, 8, 128), F32),
        pltpu.VMEM((4, low, half), F32),
        dma((CHUNKS, 3)), dma((2,)), dma((2,)), dma((2,)), dma((4,)),
        dma((n_fs - 1, 2)), dma((n_fs - 1, 2)),
        dma((n_fs - 1, n_rep - 1, 2)), dma((n_fs - 1, n_rep - 1, 2)),
    ]
    for count in (n_rep, n_fs, n_rep, n_fs, n_rep, n_tp):
        scratch += [dma((count - 1,)), dma((count - 1,))]
    value_rows, gate_rows, scaled, projected, squares = pl.pallas_call(
        functools.partial(exchange, n_fs, n_rep, n_tp),
        out_shape=(
            jax.ShapeDtypeStruct((rows * n_fs, half), BF16),
            jax.ShapeDtypeStruct((rows * n_fs, half), BF16),
            jax.ShapeDtypeStruct((n_rep, rank, width), BF16),
            jax.ShapeDtypeStruct((n_rep, low, width), BF16),
            jax.ShapeDtypeStruct((2, 8, 128), F32),
        ),
        in_specs=[any_spec] * 11,
        out_specs=(any_spec, any_spec, vmem, vmem, vmem),
        scratch_shapes=scratch,
        compiler_params=pltpu.CompilerParams(
            collective_id=0, has_side_effects=True, vmem_limit_bytes=52 * 1024 * 1024
        ),
        name="exchange",
    )(*args)

    block = min(rows, 256)
    own_blocks = rows // block
    blocks = model // block
    where = (lax.axis_index("fs") * own_blocks).astype(jnp.int32).reshape(1)

    def turned(i, w):
        return (lax.rem(w[0] + i, blocks), 0)

    def own(i, w):
        return (jnp.minimum(i, own_blocks - 1), 0)

    def whole(shape):
        return pl.BlockSpec(shape, lambda i, w: (0,) * len(shape))

    row_spec = pl.BlockSpec((block, half), turned)
    basis_spec = pl.BlockSpec((block, rank), turned)
    own_spec = pl.BlockSpec((block, half), own)
    moment = whole((low, half))
    return pl.pallas_call(
        functools.partial(finish, own_blocks, float(model) * half * n_tp),
        grid_spec=pltpu.PrefetchScalarGridSpec(
            num_scalar_prefetch=1,
            grid=(blocks,),
            in_specs=[row_spec, row_spec, basis_spec, basis_spec, own_spec, own_spec,
                      whole(scaled.shape), whole(projected.shape), whole(squares.shape)] + [moment] * 4,
            out_specs=[own_spec, own_spec, row_spec, row_spec, own_spec, own_spec] + [moment] * 4,
        ),
        out_shape=[
            jax.ShapeDtypeStruct((rows, half), F32),
            jax.ShapeDtypeStruct((rows, half), F32),
            jax.ShapeDtypeStruct((model, half), BF16),
            jax.ShapeDtypeStruct((model, half), BF16),
            jax.ShapeDtypeStruct((rows, half), F32),
            jax.ShapeDtypeStruct((rows, half), F32),
        ] + [jax.ShapeDtypeStruct((low, half), F32)] * 4,
        compiler_params=pltpu.CompilerParams(vmem_limit_bytes=40 * 1024 * 1024),
        name="finish",
    )(where, value_rows, gate_rows, value_basis, gate_basis, value_weight, gate_weight,
      scaled, projected, squares, value_first, gate_first, value_second, gate_second)


def solution(mesh):
    sizes = tuple(mesh.shape[name] for name in ("fs", "rep", "tp"))
    return jax.shard_map(
        lambda *args: tuple(local(sizes, *args)),
        mesh=mesh,
        in_specs=(
            P(("fs", "rep"), None),
            P(("fs", "rep"), "tp"),
            P(("fs", "rep"), "tp"),
            P("fs", "tp"),
            P("fs", "tp"),
            P(),
            P(),
            P("fs", "tp"),
            P("fs", "tp"),
            P("fs", "tp"),
            P("fs", "tp"),
        ),
        out_specs=(
            P("fs", "tp"),
            P("fs", "tp"),
            P(None, "tp"),
            P(None, "tp"),
            P("fs", "tp"),
            P("fs", "tp"),
            P("fs", "tp"),
            P("fs", "tp"),
            P("fs", "tp"),
            P("fs", "tp"),
        ),
        check_vma=False,
    )
```
